512 devices in a mesh: sp: 32 (over z, core), tp: 16 (over y, x).
Axes of the slice: x: 4, y: 4, z: 16, core: 2. Of those that a mesh axis runs over, the one named last changes fastest.
Arguments:
- query_heads: bfloat16 [8192, 1024], P('sp', 'tp'), may hold values from -6 to 6
- key_heads: bfloat16 [8192, 256], P('sp'), may hold values from -6 to 6
- value_heads: bfloat16 [8192, 256], P('sp'), may hold values from -24 to 24
- q_gain: float32 [64], replicated, may hold values from 0.6 to 4.5
- k_gain: float32 [64], replicated, may hold values from 0.6 to 4.5
- out_weight: bfloat16 [1024, 2048], P('tp'), may hold values from -0.1875 to 0.1875
- residual: bfloat16 [8192, 2048], P('sp', 'tp'), may hold values from -3 to 3
- norm_gain: float32 [2048], P('tp'), may hold values from 0.1 to 1.9
- routes: int32 [8192, 2], P('sp'), may hold values from 0 to 31, all different within a row; in each aligned block of 256 rows (0 to 255, 256 to 511, ...) at most 21 rows name the same one
- route_weights: float32 [8192, 2], P('sp'), may hold values from 0.5 to 1.5
- w_gate: bfloat16 [32, 2048, 4096], P('sp', None, 'tp'), may hold values from -0.125 to 0.125
- w_up: bfloat16 [32, 2048, 4096], P('sp', None, 'tp'), may hold values from -0.125 to 0.125
- w_down: bfloat16 [32, 4096, 2048], P('sp', 'tp'), may hold values from -0.1875 to 0.1875
Outputs:
- layer_out: bfloat16 [8192, 2048], P('sp', 'tp')
The draws below stay inside these ranges and needn't reach their ends.
Inputs may be any that keep to these rules, and one draw needn't show every extreme that they name: `routes`: each row names 2 different experts. Among the 256 rows of one index of sp, no expert is named more than 21 times, a bound that some block reaches.
All inputs are finite; a program needn't handle non-finite values.
Results may differ from the reference program's by a relative error of at most 0.02.
The reference program's roundings to bfloat16 on the way count: a program that leaves them out, or rounds other values in their place, can miss the bound.
Values may be sent and summed in bfloat16 or wider, within the bound.
A program may use at most 64 MiB of HBM per device.

```python
import math
import jax
import jax.numpy as jnp
import numpy as np
from jax import lax

D = 2048
HQ = 16
KV = 4
E = 64
FF = 4096
TOPK = 2
GRID_W = 64
TOK_SP = 256
TOKENS = 8192
EXPERTS = 32
CAP = 21
N_SP = 32
N_TP = 16


def base_keys(key):
    drawn = jax.random.normal(jax.random.fold_in(key, 11), (TOKENS, KV * E), jnp.float32)
    return jnp.clip(drawn, -6.0, 6.0)


def draw_key_heads(key, part):
    return base_keys(key).astype(jnp.bfloat16)


def draw_query_heads(key, part):
    fresh = jax.random.normal(jax.random.fold_in(key, 23), (TOKENS, KV, HQ // KV, E), jnp.float32)
    fresh = jnp.clip(fresh, -6.0, 6.0)
    return fresh.reshape(TOKENS, HQ * E).astype(jnp.bfloat16)


def gain_of(key, salt):
    return 1.0 + 0.18 * jax.random.uniform(jax.random.fold_in(key, salt), (E,), jnp.float32, -2.0, 2.0)


def draw_q_gain(key, part):
    return gain_of(key, 31)


def draw_k_gain(key, part):
    return gain_of(key, 37)


def draw_residual(key, part):
    noise_key = jax.random.fold_in(key, 41)
    row_key = jax.random.fold_in(key, 43)
    column_pos = jnp.arange(D, dtype=jnp.float32) / D
    row_scale = jnp.exp(jax.random.uniform(row_key, (TOKENS, 1), jnp.float32, 0.0, jnp.log(2.0)))
    base = jax.random.normal(noise_key, (TOKENS, D), jnp.float32)
    column_scale = 0.05 * jnp.exp(jnp.log(10.0) * column_pos)
    values = base * row_scale * column_scale[None, :]
    return jnp.clip(values, -3.0, 3.0).astype(jnp.bfloat16)


def steps_of(rng, dims, shards, smallest, top_value):
    level = 1.0
    for axis_at, shards_of in shards:
        steps = jax.random.uniform(jax.random.fold_in(jax.random.fold_in(rng, 6), axis_at), (shards_of,), jnp.float32, smallest / len(shards), top_value / len(shards))
        level = level * jnp.repeat(jnp.exp(steps), dims[axis_at] // shards_of).reshape((-1,) + (1,) * (len(dims) - 1 - axis_at))
    return level


def deal_out(key, own, number, rows, count, top, most, slope):
    order = jax.random.permutation(key, count)
    crowded, common = load_shares(count, rows * top, most, slope, True), load_shares(count, rows * top, most, slope, False)
    places = jnp.arange(count)

    def named(tallies, turn):
        used = int((tallies > 0).sum())
        fixed = max(1, used // 4)
        shifted = fixed + (places - fixed + turn * (used - fixed)) % max(1, count - fixed)
        return jnp.zeros((count,), jnp.int32).at[order[jnp.where(places < fixed, places, shifted)]].set(jnp.asarray(tallies, jnp.int32))

    tallies = jnp.where(number % 4 == 0, named(crowded, number // 4), named(common, number - number // 4 - 1))
    mixed = jax.random.permutation(jax.random.fold_in(own, 3), count)
    giver, receiver = mixed[0:count // 2 * 2:2], mixed[1:count // 2 * 2:2]
    room = jnp.minimum(tallies[giver] - 1, most - tallies[receiver]) // 2
    room = jnp.where((giver == order[0]) | (receiver == order[0]) | (tallies[receiver] == 0), 0, jnp.maximum(room, 0))
    shifted = jax.random.randint(jax.random.fold_in(own, 4), (count // 2,), 0, 1 << 20) % (room + 1)
    tallies = tallies.at[giver].add(-shifted).at[receiver].add(shifted)
    labels = jnp.searchsorted(jnp.cumsum(tallies), jnp.arange(rows * top), side="right").astype(jnp.int32)
    table = labels.reshape(top, rows).T
    table = table[jax.random.permutation(jax.random.fold_in(own, 1), rows)]
    turn = jax.random.randint(jax.random.fold_in(own, 2), (rows, 1), 0, top)
    return jnp.take_along_axis(table, (jnp.arange(top)[None, :] + turn) % top, axis=1)


def load_shares(amount, total, bound, lean, full):
    portions = [(1 << 20) // math.isqrt(rank ** lean) + 1 for rank in range(1, amount + 1)]
    largest = bound if full else min(bound, max(-(-total // amount), total * portions[0] // sum(portions)))
    least = 1 if total - largest >= amount - 1 else 0
    holding, spare = [largest] + [least] * (amount - 1), total - largest - least * (amount - 1)
    while spare > 0:
        movable = [i for i in range(1, amount) if holding[i] < largest] or [i for i in range(1, amount) if holding[i] < bound]
        mass, remaining = sum([portions[i] for i in movable]), spare
        for i in movable:
            addition = min(bound - holding[i], max(1, remaining * portions[i] // mass), spare)
            holding[i] = holding[i] + addition
            spare = spare - addition
    return np.array(holding)


def normal_values(stream_key, dims, scale, bound, cuts=(), kind=jnp.bfloat16):
    level = steps_of(stream_key, dims, cuts, -0.22, 0.18) if cuts else 1.0
    array = jax.random.normal(stream_key, dims, jnp.float32) * scale * level
    return jnp.minimum(jnp.maximum(array, -bound), bound).astype(kind)


def setup_inputs(seed: int = 0) -> dict:
    arg_keys = jax.random.split(jax.random.key(seed), 14)
    query_heads = draw_query_heads(jax.random.fold_in(arg_keys[13], 71), 0)
    key_heads = draw_key_heads(jax.random.fold_in(arg_keys[13], 71), 0)
    value_heads = normal_values(arg_keys[2], (TOKENS, KV * E), 4.0, 24.0, ((0, 32),))
    q_gain = draw_q_gain(jax.random.fold_in(arg_keys[13], 71), 0)
    k_gain = draw_k_gain(jax.random.fold_in(arg_keys[13], 71), 0)
    out_weight = normal_values(arg_keys[5], (HQ * E, D), (HQ * E) ** -0.5, 0.1875, ((0, 16),))
    residual = draw_residual(jax.random.fold_in(arg_keys[13], 71), 0)
    norm_gain = jnp.clip(1.0 + 0.18 * jax.random.normal(arg_keys[7], (D,), jnp.float32), 0.1, 1.9)
    routes_keys = jax.random.split(jax.random.fold_in(arg_keys[8], 1), TOKENS // TOK_SP)
    routes_turns = jax.random.permutation(jax.random.fold_in(arg_keys[8], 3), TOKENS // TOK_SP)
    routes = jax.vmap(lambda own, number: deal_out(jax.random.fold_in(arg_keys[8], 2), own, number, TOK_SP, EXPERTS, TOPK, CAP, 1))(routes_keys, routes_turns).reshape((TOKENS, TOPK))
    route_weights = jnp.clip(0.5 + 1.0 * jax.random.uniform(arg_keys[9], (TOKENS, TOPK), jnp.float32) ** steps_of(arg_keys[9], (TOKENS, TOPK), ((0, 32),), -0.2, 0.2), 0.5, 1.5)
    w_gate = normal_values(arg_keys[10], (EXPERTS, D, FF), D ** -0.5, 0.125, ((0, 32), (2, 16)))
    w_up = normal_values(arg_keys[11], (EXPERTS, D, FF), D ** -0.5, 0.125, ((0, 32), (2, 16)))
    w_down = normal_values(arg_keys[12], (EXPERTS, FF, D), (FF // 4) ** -0.5, 0.1875, ((0, 32), (1, 16)))
    return {"query_heads": query_heads, "key_heads": key_heads, "value_heads": value_heads, "q_gain": q_gain, "k_gain": k_gain, "out_weight": out_weight, "residual": residual, "norm_gain": norm_gain, "routes": routes, "route_weights": route_weights, "w_gate": w_gate, "w_up": w_up, "w_down": w_down}


norm_eps = 1e-06
rope_base = 10000.0

def normalize(values_f, gain):
    mean_sq = lax.optimization_barrier(jnp.mean(values_f * values_f, axis=-1, keepdims=True))
    return values_f * lax.rsqrt(mean_sq + norm_eps) * gain

def rotate(values_f, positions):
    head_width = values_f.shape[-1]
    half_width = head_width // 2
    quarter_width = half_width // 2
    frequency = rope_base ** (-jnp.arange(quarter_width, dtype=jnp.float32) / quarter_width)
    grid_rows = (positions // GRID_W).astype(jnp.float32)
    grid_cols = (positions % GRID_W).astype(jnp.float32)
    shape = (values_f.shape[0],) + (1,) * (values_f.ndim - 2) + (quarter_width,)
    pieces = []
    for coords, offset_lo in ((grid_rows, 0), (grid_cols, half_width)):
        angles = coords[:, None] * frequency[None, :]
        cosine = jnp.cos(angles).reshape(shape)
        sines = jnp.sin(angles).reshape(shape)
        first_part = values_f[..., offset_lo:offset_lo + quarter_width]
        second_part = values_f[..., offset_lo + quarter_width:offset_lo + half_width]
        pieces.append(first_part * cosine - second_part * sines)
        pieces.append(second_part * cosine + first_part * sines)
    return jnp.concatenate(pieces, axis=-1)

def slots_of(assign):
    onehot = (assign[:, None] == jnp.arange(EXPERTS, dtype=jnp.int32)[None, :]).astype(jnp.int32)
    before = jnp.cumsum(onehot, axis=0) - onehot
    return lax.optimization_barrier(jnp.sum(before * onehot, axis=1)).astype(jnp.int32)

def reference(query_heads, key_heads, value_heads, q_gain, k_gain, out_weight, residual, norm_gain, routes, route_weights, w_gate, w_up, w_down):
    group_size = HQ // KV
    positions = jnp.arange(TOKENS, dtype=jnp.int32)
    query_f = query_heads.astype(jnp.float32).reshape(TOKENS, KV, group_size, E)
    q_turned = rotate(normalize(query_f, q_gain), positions).astype(jnp.bfloat16)
    key_f = key_heads.astype(jnp.float32).reshape(TOKENS, KV, E)
    k_turned = rotate(normalize(key_f, k_gain), positions).astype(jnp.bfloat16).astype(jnp.float32)
    value_f = value_heads.astype(jnp.float32).reshape(TOKENS, KV, E)

    def query_block(block_q):
        scores = jnp.einsum('qcge,kce->cgqk', block_q.astype(jnp.float32), k_turned) * E ** (-0.5)
        row_max = lax.optimization_barrier(jnp.max(scores, axis=-1, keepdims=True))
        exped = jnp.exp(scores - row_max)
        denominator = lax.optimization_barrier(jnp.sum(exped, axis=-1))
        rounded = lax.optimization_barrier(exped.astype(jnp.bfloat16))
        weighted = jnp.einsum('cgqk,kce->qcge', rounded.astype(jnp.float32), value_f)
        return (weighted / jnp.transpose(denominator, (2, 0, 1))[..., None]).astype(jnp.bfloat16)
    attended = lax.map(query_block, q_turned.reshape(N_SP, TOK_SP, KV, group_size, E))
    attended = attended.reshape(TOKENS, HQ * E)
    rows_tp = HQ * E // N_TP
    head_blocks = attended.reshape(TOKENS, N_TP, rows_tp).transpose(1, 0, 2)
    weight_blocks = out_weight.reshape(N_TP, rows_tp, D)

    def add_block(running, operands):
        partial_value = jnp.dot(operands[0], operands[1], preferred_element_type=jnp.float32).astype(jnp.bfloat16)
        partial_value = lax.optimization_barrier(partial_value)
        return (running + partial_value.astype(jnp.float32), None)
    attn_out, _ = lax.scan(add_block, jnp.zeros((TOKENS, D), jnp.float32), (head_blocks, weight_blocks))
    after_attn = residual.astype(jnp.float32) + attn_out
    mean_sq = lax.optimization_barrier(jnp.mean(after_attn * after_attn, axis=1, keepdims=True))
    normed = (after_attn * lax.rsqrt(mean_sq + norm_eps) * norm_gain).astype(jnp.bfloat16)
    assign = routes.reshape(N_SP, TOK_SP * TOPK)
    slot_rank = jax.vmap(slots_of)(assign)
    slot_index = assign * CAP + slot_rank
    token_local = (jnp.arange(TOK_SP * TOPK, dtype=jnp.int32) // TOPK).astype(jnp.int32)

    def table_of(indices):
        return jnp.full((EXPERTS * CAP,), TOK_SP, jnp.int32).at[indices].set(token_local)
    slot_token = jax.vmap(table_of)(slot_index)
    group_start = (jnp.arange(N_SP, dtype=jnp.int32) * TOK_SP)[:, None]
    global_token = jnp.where(slot_token < TOK_SP, slot_token + group_start, TOKENS).astype(jnp.int32)
    row_index = global_token.reshape(N_SP, EXPERTS, CAP).transpose(1, 0, 2).reshape(EXPERTS, N_SP * CAP)
    padded = jnp.concatenate([normed, jnp.zeros((1, D), jnp.bfloat16)], axis=0)
    hidden_tp = FF // N_TP

    def expert(operands):
        indices, gate_w, up_w, down_w = operands
        gathered = padded[indices]
        gate_sum = jnp.dot(gathered, gate_w, preferred_element_type=jnp.float32)
        up_sum = jnp.dot(gathered, up_w, preferred_element_type=jnp.float32)
        activated = (jax.nn.silu(gate_sum) * up_sum).astype(jnp.bfloat16)
        act_blocks = activated.reshape(N_SP * CAP, N_TP, hidden_tp).transpose(1, 0, 2)
        down_blocks = down_w.reshape(N_TP, hidden_tp, D)

        def add_part(running, pair):
            partial_value = jnp.dot(pair[0], pair[1], preferred_element_type=jnp.float32).astype(jnp.bfloat16)
            partial_value = lax.optimization_barrier(partial_value)
            return (running + partial_value.astype(jnp.float32), None)
        total, _ = lax.scan(add_part, jnp.zeros((N_SP * CAP, D), jnp.float32), (act_blocks, down_blocks))
        return total.astype(jnp.bfloat16)
    expert_rows = lax.map(expert, (row_index, w_gate, w_up, w_down)).reshape(EXPERTS, N_SP, CAP, D)
    group_idx = jnp.arange(N_SP, dtype=jnp.int32)[:, None]
    picked = expert_rows[assign, group_idx, slot_rank].astype(jnp.float32)
    picked = picked.reshape(TOKENS, TOPK, D)
    expert_mix = lax.optimization_barrier(jnp.sum(picked * route_weights[:, :, None], axis=1))
    return (after_attn + expert_mix).astype(jnp.bfloat16)
```

```python
import functools
import jax
import jax.numpy as jnp
import numpy as np
from jax import lax
from jax.experimental import pallas as pl
from jax.experimental.pallas import tpu as pltpu
from jax.sharding import Mesh
from jax.sharding import PartitionSpec as P

D = 2048
HQ = 16
KV = 4
E = 64
TOPK = 2
GRID_W = 64
CAP = 21
TOK = 256
LANES = 128
norm_eps = 1e-06
rope_base = 10000.0
MESH = pl.DeviceIdType.MESH


def rope_tables(n_rows):
    quarter = E // 4
    freq = (rope_base ** (-np.arange(quarter, dtype=np.float32) / quarter)).astype(np.float32)
    out = []
    for count, lo in ((n_rows, 0), (GRID_W, E // 2)):
        ang = np.arange(count, dtype=np.float32)[:, None] * freq[None, :]
        cos = np.zeros((count, LANES), np.float32)
        sin = np.zeros((count, LANES), np.float32)
        c, s = np.cos(ang), np.sin(ang)
        cos[:, lo : lo + quarter] = c
        cos[:, lo + quarter : lo + 2 * quarter] = c
        sin[:, lo : lo + quarter] = -s
        sin[:, lo + quarter : lo + 2 * quarter] = s
        if lo:
            cos[:, E:] = 1.0
        out += [cos, sin]
    return out


def attention_kernel(nz, tp_of, q_ref, k_ref, v_ref, qg_ref, kg_ref, rc_ref, rs_ref, cc_ref, cs_ref,
                     out_ref, kv, qt, q128, gains, cos_t, sin_t, m_ref, l_ref, acc,
                     send, recv, dsend, drecv):
    sp = lax.axis_index("sp")
    head = tp_of() // (HQ // KV)
    core = lax.rem(sp, 2)
    up = lax.rem(sp + 2, 2 * nz)
    down = lax.rem(sp + 2 * nz - 2, 2 * nz)
    partner = sp + 1 - 2 * core
    half = nz // 2

    barrier = pltpu.get_barrier_semaphore()
    for other in (up, down, partner):
        pl.semaphore_signal(barrier, inc=1, device_id={"sp": other}, device_id_type=MESH)

    lane = lax.broadcasted_iota(jnp.int32, (TOK, LANES), 1)
    low = lane < E
    rows_per = TOK // GRID_W
    for g in range(rows_per):
        at = pl.ds(g * GRID_W, GRID_W)
        cos_t[at, :] = cc_ref[...] + rc_ref[pl.ds(sp * rows_per + g, 1), :]
        sin_t[at, :] = cs_ref[...] + rs_ref[pl.ds(sp * rows_per + g, 1), :]
    gains[...] = jnp.ones_like(gains)
    gains[0:1, 0:E] = qg_ref[...]
    gains[1:2, 0:E] = kg_ref[...]

    def turned(x, gain):
        sq = jnp.where(low, x * x, 0.0)
        mean_sq = jnp.sum(sq, axis=1, keepdims=True) / E
        x = jnp.where(low, x * lax.rsqrt(mean_sq + norm_eps) * gain, x)
        swapped = jnp.where(
            lax.rem(lane, 32) < 16, pltpu.roll(x, LANES - 16, 1), pltpu.roll(x, 16, 1)
        )
        return x * cos_t[...] + swapped * sin_t[...]

    def tile_of(ref):
        return jnp.where(
            head >= 2, ref[:, LANES : 2 * LANES].astype(jnp.float32), ref[:, 0:LANES].astype(jnp.float32)
        )

    odd = lax.rem(head, 2) == 1
    kt = tile_of(k_ref)
    vt = tile_of(v_ref)
    k_lo = jnp.where(odd, pltpu.roll(kt, E, 1), kt)
    v_hi = jnp.where(odd, vt, pltpu.roll(vt, E, 1))
    kv[0, 0:TOK, :] = turned(jnp.where(low, k_lo, v_hi), gains[1:2, :]).astype(jnp.bfloat16)

    pl.semaphore_wait(barrier, 3)

    def unit(s, d):
        return 2 * s - 1 + d

    HB = TOK // 2

    def hop(s, d, h, src_u, dst_u):
        return pltpu.make_async_remote_copy(
            src_ref=kv.at[src_u, pl.ds(h * HB, HB)],
            dst_ref=kv.at[dst_u, pl.ds(h * HB, HB)],
            send_sem=send.at[s, d, h],
            recv_sem=recv.at[s, d, h],
            device_id={"sp": up if d == 0 else down},
            device_id_type=MESH,
        )

    def across(u):
        return pltpu.make_async_remote_copy(
            src_ref=kv.at[u, pl.ds(0, TOK)],
            dst_ref=kv.at[u, pl.ds(TOK, TOK)],
            send_sem=dsend.at[u],
            recv_sem=drecv.at[u],
            device_id={"sp": partner},
            device_id_type=MESH,
        )

    last = 2 * half - 1
    for h in range(2):
        for d in range(2):
            hop(1, d, h, 0, unit(1, d)).start()
    across(0).start()

    q128[...] = jnp.zeros_like(q128)
    q128[:, 0:E] = q_ref[...].astype(jnp.float32)
    q_rot = turned(q128[...], gains[0:1, :]) * (E ** -0.5)
    qt[...] = q_rot.T.astype(jnp.bfloat16)
    m_ref[...] = jnp.full_like(m_ref, -1e30)
    l_ref[...] = jnp.zeros_like(l_ref)
    acc[...] = jnp.zeros_like(acc)

    def attend(u):
        block = kv[u]
        s = jnp.dot(block, qt[...], preferred_element_type=jnp.float32)
        m_old = m_ref[...]
        m_new = jnp.maximum(m_old, jnp.max(s, axis=0, keepdims=True))
        alpha = jnp.exp(m_old - m_new)
        p = jnp.exp(s - m_new)
        l_ref[...] = l_ref[...] * alpha + jnp.sum(p, axis=0, keepdims=True)
        acc[...] = acc[...] * alpha + lax.dot_general(
            block, p.astype(jnp.bfloat16), (((0,), (0,)), ((), ())), preferred_element_type=jnp.float32
        )
        m_ref[...] = m_new

    def arrive(s, forward):
        for h in range(2):
            for d in range(2):
                hop(s, d, h, 0, unit(s, d)).wait_recv()
                forward(d, h)
        for d in range(2):
            across(unit(s, d)).start()

    def step(s, carry):
        def forward(d, h):
            hop(s + 1, d, h, unit(s, d), unit(s + 1, d)).start()

        arrive(s, forward)

        @pl.when(s == 1)
        def _():
            across(0).wait_recv()
            attend(0)

        @pl.when(s > 1)
        def _():
            for d in range(2):
                u = unit(s - 1, d)
                across(u).wait_recv()
                attend(u)

        return carry

    lax.fori_loop(1, half - 1, step, 0)

    def forward_last(d, h):
        if d == h:
            hop(half, d, h, unit(half - 1, d), last).start()

    arrive(half - 1, forward_last)
    for d in range(2):
        u = unit(half - 2, d)
        across(u).wait_recv()
        attend(u)
    for d in range(2):
        hop(half, d, d, 0, last).wait_recv()
    across(last).start()
    for d in range(2):
        u = unit(half - 1, d)
        across(u).wait_recv()
        attend(u)
    across(last).wait_recv()
    attend(last)
    out_ref[...] = (acc[E:, :] / l_ref[...]).astype(jnp.bfloat16)

    def drain(s, carry):
        for h in range(2):
            for d in range(2):
                hop(s, d, h, 0, unit(s, d)).wait_send()
        return carry

    lax.fori_loop(1, half, drain, 0)
    for d in range(2):
        hop(half, d, d, 0, last).wait_send()

    def drain_across(u, carry):
        across(u).wait_send()
        return carry

    lax.fori_loop(0, last + 1, drain_across, 0)


def attention(nz, tp_of, query_heads, key_heads, value_heads, q_gain, k_gain):
    tables = [jnp.asarray(t) for t in rope_tables(nz * 2 * TOK // GRID_W)]
    units = nz
    vmem = pl.BlockSpec(memory_space=pltpu.VMEM)
    return pl.pallas_call(
        functools.partial(attention_kernel, nz, tp_of),
        out_shape=jax.ShapeDtypeStruct((E, TOK), jnp.bfloat16),
        in_specs=[vmem] * 9,
        out_specs=vmem,
        scratch_shapes=[
            pltpu.VMEM((units, 2 * TOK, LANES), jnp.bfloat16),
            pltpu.VMEM((LANES, TOK), jnp.bfloat16),
            pltpu.VMEM((TOK, LANES), jnp.float32),
            pltpu.VMEM((8, LANES), jnp.float32),
            pltpu.VMEM((TOK, LANES), jnp.float32),
            pltpu.VMEM((TOK, LANES), jnp.float32),
            pltpu.VMEM((1, TOK), jnp.float32),
            pltpu.VMEM((1, TOK), jnp.float32),
            pltpu.VMEM((LANES, TOK), jnp.float32),
            pltpu.SemaphoreType.DMA((nz // 2 + 1, 2, 2)),
            pltpu.SemaphoreType.DMA((nz // 2 + 1, 2, 2)),
            pltpu.SemaphoreType.DMA((units,)),
            pltpu.SemaphoreType.DMA((units,)),
        ],
        compiler_params=pltpu.CompilerParams(collective_id=0, has_side_effects=True),
        cost_estimate=pl.CostEstimate(flops=10**9, bytes_accessed=2 * 10**6, transcendentals=0),
    )(query_heads, key_heads, value_heads, q_gain.reshape(1, E), k_gain.reshape(1, E), *tables)


TP = ("tp_0", "tp_1")


def cut_along(array, dim, peers):
    dims = array.shape
    tiles = array.reshape(*dims[:dim], peers, dims[dim] // peers, *dims[dim + 1 :])
    return jnp.moveaxis(tiles, dim, 0)


def sum_at_owner(array, axis, dim):
    peers = lax.axis_size(axis)
    tiles = lax.all_to_all(cut_along(array, dim, peers), axis, 0, 0, tiled=True)
    return jnp.sum(tiles.astype(jnp.float32), axis=0)


def by_axis(array, axes):
    for axis in axes:
        array = lax.psum(array, axis)
    return array


def gather_axes(array, axes, dim):
    if not axes:
        return array
    nearer = lax.all_gather(array, axes[-1], axis=dim, tiled=True)
    return gather_axes(nearer, axes[:-1], dim)


def shards(
    query_heads,
    key_heads,
    value_heads,
    q_gain,
    k_gain,
    out_weight,
    residual,
    norm_gain,
    routes,
    route_weights,
    w_gate,
    w_up,
    w_down,
):
    tok_rows = query_heads.shape[0]
    tok_rows = query_heads.shape[0]
    nz = lax.axis_size("sp") // 2
    attended_t = attention(nz, lambda: lax.axis_index(TP), query_heads, key_heads, value_heads, q_gain, k_gain)
    attended = attended_t.T
    partial_value = jnp.dot(attended, out_weight, preferred_element_type=jnp.float32).astype(
        jnp.bfloat16
    )
    attn_out = sum_at_owner(partial_value, TP, 1)
    after_attn = residual.astype(jnp.float32) + attn_out
    square_sum = by_axis(jnp.sum(after_attn * after_attn, axis=1), TP)
    normed = (after_attn * lax.rsqrt(square_sum / D + norm_eps)[:, None] * norm_gain).astype(
        jnp.bfloat16
    )
    experts_n = lax.axis_size("sp")
    capacity = 5 * tok_rows * TOPK // (4 * experts_n) + 1
    assign = routes.reshape(tok_rows * TOPK)
    onehot = (assign[:, None] == jnp.arange(experts_n, dtype=jnp.int32)[None, :]).astype(jnp.int32)
    before = jnp.cumsum(onehot, axis=0) - onehot
    slot_rank = jnp.sum(before * onehot, axis=1)
    slot_index = assign * capacity + slot_rank
    token_local = jnp.arange(tok_rows * TOPK, dtype=jnp.int32) // TOPK
    slot_token = (
        jnp.full((experts_n * capacity,), tok_rows, jnp.int32).at[slot_index].set(token_local)
    )
    gate_w = w_gate[0]
    up_w = w_up[0]
    down_w = w_down[0]
    padded = jnp.concatenate([normed, jnp.zeros((1, normed.shape[1]), jnp.bfloat16)], axis=0)
    slot_rows = padded[slot_token].reshape(experts_n, capacity, normed.shape[1])
    block_rows = gather_axes(
        lax.all_to_all(slot_rows, "sp", split_axis=0, concat_axis=0, tiled=True), TP, 2
    )
    gate_next = jnp.einsum("scd,df->scf", block_rows, gate_w, preferred_element_type=jnp.float32)
    up_next = jnp.einsum("scd,df->scf", block_rows, up_w, preferred_element_type=jnp.float32)
    activated = (jax.nn.silu(gate_next) * up_next).astype(jnp.bfloat16)
    partials = jnp.einsum(
        "scf,fd->scd", activated, down_w, preferred_element_type=jnp.float32
    ).astype(jnp.bfloat16)
    expert_rows = sum_at_owner(partials, TP, 2).astype(jnp.bfloat16)
    returned_rows = lax.all_to_all(expert_rows, "sp", split_axis=0, concat_axis=0, tiled=True)
    columns = returned_rows.shape[2]
    picked = returned_rows.reshape(experts_n * capacity, columns)[slot_index].astype(jnp.float32)
    picked = picked.reshape(tok_rows, TOPK, columns)
    expert_mix = jnp.sum(picked * route_weights[:, :, None], axis=1)
    return (after_attn + expert_mix).astype(jnp.bfloat16)


def solution(mesh):
    finer = Mesh(mesh.devices.reshape(mesh.shape["sp"], 4, 4), ("sp", "tp_0", "tp_1"))
    in_specs = (
        P("sp", TP),
        P("sp", None),
        P("sp", None),
        P(),
        P(),
        P(TP, None),
        P("sp", TP),
        P(TP),
        P("sp", None),
        P("sp", None),
        P("sp", None, TP),
        P("sp", None, TP),
        P("sp", TP, None),
    )
    out_specs = P("sp", TP)
    return jax.shard_map(
        shards, mesh=finer, in_specs=in_specs, out_specs=out_specs, check_vma=False
    )
```
